32 devices in a mesh: grp: 2 (over y), sp: 4 (over z), tp: 4 (over x, core).
Axes of the slice: x: 2, y: 2, z: 4, core: 2. Of those that a mesh axis runs over, the one named last changes fastest.
Arguments:
- tokens: bfloat16 [2048, 4096], P(('grp', 'sp'), 'tp'), parts along dimension 0, may hold values from -45 to 45
- norm_gain: float32 [2, 4096], replicated, may hold values from 0.1 to 1.9
- value_weight: bfloat16 [2, 4096, 1024], P(None, 'sp', 'tp'), may hold values from -0.09375 to 0.09375
- gate_weight: bfloat16 [2, 4096, 1024], P(None, 'sp', 'tp'), may hold values from -0.09375 to 0.09375
- conv_taps: float32 [2, 31, 1024], P(None, None, 'tp'), may hold values from -4 to 4
- channel_gain: float32 [2, 1024], P(None, 'tp'), may hold values from 0.1 to 1.9
- out_weight: bfloat16 [2, 1024, 4096], P(None, 'sp', 'tp'), may hold values from -0.375 to 0.375
- final_gain: float32 [4096], P('tp'), may hold values from 0.1 to 1.9
Outputs:
- result: bfloat16 [2048, 4096], P(('grp', 'sp'), 'tp'), parts along dimension 0
The draws below stay inside these ranges and needn't reach their ends.
There are 2 independent parts, one for each index of `grp`. The reference program is written for one: setup_inputs(seed, part) draws one part's arguments, and reference() takes and returns one part's arrays. A program takes and returns all parts, laid end to end along the dimension named above; an argument that names none is the same for every part. Nothing has to cross between parts.
All inputs are finite; a program needn't handle non-finite values.
Results may differ from the reference program's by a relative error of at most 0.012.
Values may be sent and summed in bfloat16 or wider, within the bound.
A program may use at most 128 MiB of HBM per device.

```python
import jax
import jax.numpy as jnp
from jax import lax

D = 4096
C = 1024
KERNEL = 31
LAYERS = 2
TOKENS = 1024


def draw_tokens(key, part):
    key_base, key_cols, key_rows = jax.random.split(key, 3)
    cols = jnp.arange(D, dtype=jnp.float32) / D
    col_scale = jnp.exp(jnp.log(3.0) * cols) * jnp.exp(jax.random.uniform(key_cols, (D,), jnp.float32, -0.35, 0.35))
    row_scale = jnp.exp(jax.random.uniform(key_rows, (TOKENS, 1), jnp.float32, -0.69, 0.69))
    base = jnp.clip(jax.random.normal(key_base, (TOKENS, D), jnp.float32), -4.0, 4.0)
    return (base * col_scale[None, :] * row_scale).astype(jnp.bfloat16)


def draw_conv_taps(key, part):
    key_base, key_cols = jax.random.split(key, 2)
    cols = jnp.arange(C, dtype=jnp.float32) / C
    col_scale = jnp.exp(jnp.log(3.0) * cols) * jnp.exp(jax.random.uniform(key_cols, (LAYERS, 1, C), jnp.float32, -0.5, 0.5))
    base = jnp.clip(jax.random.normal(key_base, (LAYERS, KERNEL, C), jnp.float32), -4.0, 4.0)
    return base * col_scale * KERNEL ** (-0.5)


def levels(key, shape, cuts, low, top_value):
    factor_of, own = 1.0, jax.random.fold_in(key, 6)
    for position, parts in cuts:
        steps = jnp.exp(jax.random.uniform(jax.random.fold_in(own, position), (parts,), jnp.float32, low / len(cuts), top_value / len(cuts)))
        factor_of = factor_of * jnp.repeat(steps, shape[position] // parts).reshape([-1 if axis == position else 1 for axis in range(len(shape))])
    return factor_of


def noise(own_key, dims, scale, most, pieces=(), held_as=jnp.bfloat16):
    entries = scale * jax.random.normal(own_key, dims, jnp.float32)
    if pieces:
        entries = entries * levels(own_key, dims, pieces, -0.22, 0.18)
    return jnp.clip(entries, -most, most).astype(held_as)


def setup_inputs(seed: int = 0, part: int = 0) -> dict:
    keys = jax.random.split(jax.random.key(seed), 9)
    part_keys = jax.random.split(jax.random.fold_in(keys[8], part), 9)
    return {
        "tokens": draw_tokens(jax.random.fold_in(jax.random.fold_in(keys[8], part), 71), part),
        "norm_gain": jnp.clip(1.0 + 0.18 * jax.random.normal(keys[1], (LAYERS, D), jnp.float32), 0.1, 1.9),
        "value_weight": noise(keys[2], (LAYERS, D, C), D ** -0.5, 0.09375, ((1, 4), (2, 4))),
        "gate_weight": noise(keys[3], (LAYERS, D, C), D ** -0.5, 0.09375, ((1, 4), (2, 4))),
        "conv_taps": draw_conv_taps(jax.random.fold_in(keys[8], 71), part),
        "channel_gain": jnp.clip(1.0 + 0.18 * jax.random.normal(keys[5], (LAYERS, C), jnp.float32), 0.1, 1.9),
        "out_weight": noise(keys[6], (LAYERS, C, D), (C // 4) ** -0.5, 0.375, ((1, 4), (2, 4))),
        "final_gain": jnp.clip(1.0 + 0.18 * jax.random.normal(keys[7], (D,), jnp.float32), 0.1, 1.9),
    }


def depthwise(glu, taps):
    reach = taps.shape[0] // 2
    padded = jnp.pad(glu.astype(jnp.float32), ((reach, reach), (0, 0)))
    length = glu.shape[0]
    total = jnp.zeros(glu.shape, jnp.float32)
    for tap in range(taps.shape[0]):
        total = total + taps[tap][None, :] * padded[tap:tap + length]
    return total

def reference(tokens, norm_gain, value_weight, gate_weight, conv_taps, channel_gain, out_weight, final_gain):
    x_state = tokens
    for layer in range(LAYERS):
        xf = x_state.astype(jnp.float32)
        scale = lax.rsqrt(lax.optimization_barrier(jnp.mean(xf * xf, axis=1, keepdims=True)) + 1e-06)
        normed = (xf * scale * norm_gain[layer][None, :]).astype(jnp.bfloat16)
        value = jnp.dot(normed, value_weight[layer], preferred_element_type=jnp.float32)
        gate = jnp.dot(normed, gate_weight[layer], preferred_element_type=jnp.float32)
        glu = (value * jax.nn.sigmoid(gate)).astype(jnp.bfloat16)
        conv = depthwise(glu, conv_taps[layer])
        center = lax.optimization_barrier(jnp.mean(conv, axis=1, keepdims=True))
        shifted = conv - center
        spread = lax.optimization_barrier(jnp.mean(shifted * shifted, axis=1, keepdims=True))
        act = jax.nn.silu(shifted * lax.rsqrt(spread + 1e-05) * channel_gain[layer][None, :]).astype(jnp.bfloat16)
        branch = jnp.dot(act, out_weight[layer], preferred_element_type=jnp.float32)
        x_state = (xf + branch).astype(jnp.bfloat16)
    xf = x_state.astype(jnp.float32)
    scale = lax.rsqrt(lax.optimization_barrier(jnp.mean(xf * xf, axis=1, keepdims=True)) + 1e-06)
    return (xf * scale * final_gain[None, :]).astype(jnp.bfloat16)
```

```python
import functools

import jax
import jax.numpy as jnp
from jax import lax
from jax.experimental import pallas as pl
from jax.experimental.pallas import tpu as pltpu
from jax.sharding import PartitionSpec as P

MESH = pl.DeviceIdType.MESH
Q = 2
PAD = 16


def kernel(
    G, n, T, L,
    tokens, gain, value_w, gate_w, taps, cgain, out_w, fgain,
    result,
    wvg, wo, xg, xn, acc, pad, padf, conv, stat, actg, x_state,
    local_sem, z_recv, right_send, left_send, y_send, y_recv,
    x_send, x_recv, a_send, a_recv, s_send, s_recv, h_send, h_recv,
):
    g, s, t = lax.axis_index("grp"), lax.axis_index("sp"), lax.axis_index("tp")
    rows, width = tokens.shape
    depth, chans = value_w.shape[1:]
    out_rows = out_w.shape[1]
    half = chans // G
    out_half = width // G
    reach = taps.shape[1] // 2
    n_taps = taps.shape[1]
    D = width * T
    C = chans * T
    chunk = depth // Q
    pieces = Q + 1
    f32, bf16 = jnp.float32, jnp.bfloat16

    def piece(p, h, j):
        layer, q = p // pieces, p % pieces
        if q < Q:
            start = pl.multiple_of(j * depth + q * chunk, chunk)
            return wvg.at[layer, h, pl.ds(start, chunk), :]
        return wo.at[layer, h, pl.ds(pl.multiple_of(j * out_rows, out_rows), out_rows), :]

    locals_ = [pltpu.make_async_copy(tokens, xg.at[0, t], local_sem.at[0])]
    own_rows = pl.ds(pl.multiple_of(s * depth, depth), depth)
    own_out = pl.ds(pl.multiple_of(s * out_rows, out_rows), out_rows)
    count = 1
    per_layer = []
    for layer in range(L):
        group = []
        for h in range(G):
            for k, w in enumerate((value_w, gate_w)):
                group.append(pltpu.make_async_copy(
                    w.at[layer, :, pl.ds(h * half, half)],
                    wvg.at[layer, h, own_rows, pl.ds(k * half, half)],
                    local_sem.at[count]))
                count += 1
            group.append(pltpu.make_async_copy(
                out_w.at[layer, :, pl.ds(h * out_half, out_half)],
                wo.at[layer, h, own_out, :], local_sem.at[count]))
            count += 1
        per_layer.append(group)
    for c in locals_ + sum(per_layer, []):
        c.start()

    barrier = pltpu.get_barrier_semaphore()
    for d in range(1, T):
        pl.semaphore_signal(barrier, inc=1, device_id={"tp": lax.rem(t + d, T)}, device_id_type=MESH)
    for d in range(1, G):
        pl.semaphore_signal(barrier, inc=1, device_id={"grp": lax.rem(g + d, G)}, device_id_type=MESH)

    @pl.when(s > 0)
    def _():
        pl.semaphore_signal(barrier, inc=1, device_id={"sp": s - 1}, device_id_type=MESH)

    @pl.when(s < n - 1)
    def _():
        pl.semaphore_signal(barrier, inc=1, device_id={"sp": s + 1}, device_id_type=MESH)

    sides = jnp.where(s > 0, 1, 0) + jnp.where(s < n - 1, 1, 0)
    pl.semaphore_wait(barrier, (T - 1) + (G - 1) + sides)

    def right(p, j):
        r = piece(p, g, j)
        return pltpu.make_async_remote_copy(
            src_ref=r, dst_ref=r, send_sem=right_send.at[p, j], recv_sem=z_recv.at[p, j],
            device_id={"sp": s + 1}, device_id_type=MESH)

    def left(p, j):
        r = piece(p, g, j)
        return pltpu.make_async_remote_copy(
            src_ref=r, dst_ref=r, send_sem=left_send.at[p, j], recv_sem=z_recv.at[p, j],
            device_id={"sp": s - 1}, device_id_type=MESH)

    def across(p, j, d, h):
        r = piece(p, h, j)
        return pltpu.make_async_remote_copy(
            src_ref=r, dst_ref=r, send_sem=y_send.at[p, j, d - 1], recv_sem=y_recv.at[p, j, d - 1],
            device_id={"grp": lax.rem(g + d, G)}, device_id_type=MESH)

    batches = []
    for layer in range(L):
        base = layer * pieces
        batches += [list(range(base, base + Q)), [base + Q]]

    def own_right(ps):
        for p in ps:
            right(p, s).start()

    def own_left(ps):
        for p in ps:
            left(p, s).start()

    def relay(b, low, high):
        low, high = min(low, n - 1), min(high, n - 1)
        following = batches[b + 1] if b + 1 < len(batches) else []

        def step(k, carry):
            for p in batches[b]:
                from_left, from_right = s - 1 - k, s + 1 + k

                @pl.when(from_left >= 0)
                def _():
                    j = jnp.maximum(from_left, 0)
                    right(p, j).wait_recv()

                    @pl.when(s < n - 1)
                    def _():
                        right(p, j).start()

                    for d in range(1, G):
                        across(p, j, d, g).start()

                @pl.when(from_right < n)
                def _():
                    j = jnp.minimum(from_right, n - 1)
                    left(p, j).wait_recv()

                    @pl.when(s > 0)
                    def _():
                        left(p, j).start()

                    for d in range(1, G):
                        across(p, j, d, g).start()

            @pl.when((k == s - 1) & (s < n - 1))
            def _():
                own_right(following)

            @pl.when((k == n - 2 - s) & (s > 0))
            def _():
                own_left(following)

            return carry

        if high > low:
            lax.fori_loop(low, high, step, 0)

    def others(fn):
        def step(j, carry):
            @pl.when(j != s)
            def _():
                fn(j)
            return carry
        lax.fori_loop(0, n, step, 0)

    def wait_across(b):
        for p in batches[b]:
            for d in range(1, G):
                others(lambda j: across(p, j, d, lax.rem(g + G - d, G)).wait_recv())

    def spread(buf, layer, send, recv):
        def copy(bit, m):
            block = buf.at[layer, t ^ m]
            return pltpu.make_async_remote_copy(
                src_ref=block, dst_ref=block, send_sem=send.at[layer, bit + m], recv_sem=recv.at[layer, bit + m],
                device_id={"tp": t ^ bit}, device_id_type=MESH)

        def arrival(bit, m):
            block = buf.at[layer, t ^ bit ^ m]
            return pltpu.make_async_remote_copy(
                src_ref=block, dst_ref=block, send_sem=send.at[layer, bit + m], recv_sem=recv.at[layer, bit + m],
                device_id={"tp": t ^ bit}, device_id_type=MESH)

        bits = []
        bit = T // 2
        while bit >= 1:
            bits.append(bit)
            bit //= 2

        def begin():
            for bit in bits:
                copy(bit, 0).start()

        def finish():
            have, sent = [0], []
            for i, bit in enumerate(bits):
                for m in have:
                    arrival(bit, m).wait_recv()
                    sent.append((bit, m))
                    for lower in bits[i + 1:]:
                        copy(lower, m ^ bit).start()
                have = have + [m ^ bit for m in have]
            return lambda: [copy(bit, m).wait_send() for bit, m in sent]

        return begin, finish

    def exchange(index, columns):
        lane = lax.broadcasted_iota(jnp.int32, (rows, 128), 1)
        tile = jnp.zeros((rows, 128), f32)
        for i, column in enumerate(columns):
            tile = jnp.where(lane == i, column, tile)
        stat[index, 0] = tile.T[:8, :]

        def copy(d):
            return pltpu.make_async_remote_copy(
                src_ref=stat.at[index, 0], dst_ref=stat.at[index, d],
                send_sem=s_send.at[index, d - 1], recv_sem=s_recv.at[index, d - 1],
                device_id={"tp": lax.rem(t + d, T)}, device_id_type=MESH)

        for d in range(1, T):
            copy(d).start()

        def total():
            for d in range(1, T):
                copy(d).wait_recv()
            sums = stat[index, 0]
            for d in range(1, T):
                sums = sums + stat[index, d]
            wide = jnp.concatenate([sums, jnp.zeros((120, rows), f32)], axis=0).T
            for d in range(1, T):
                copy(d).wait_send()
            return [wide[:, i:i + 1] for i in range(len(columns))]

        return total

    def normalize(layer):
        def squares(j, total):
            part = xg[layer, j].astype(f32)
            return total + jnp.sum(part * part, axis=1, keepdims=True)
        mean = lax.fori_loop(0, T, squares, jnp.zeros((rows, 1), f32)) / D
        scale = lax.rsqrt(mean + 1e-06)

        def body(j, carry):
            xn[j] = (xg[layer, j].astype(f32) * scale * gain[layer * T + j][None, :]).astype(bf16)
            return carry
        lax.fori_loop(0, T, body, 0)

    def project(layer):
        for h in range(G):
            def body(j, carry):
                block = wvg[layer, h, pl.ds(pl.multiple_of(j * width, width), width), :]
                part = jnp.dot(xn[j], block, preferred_element_type=f32)

                @pl.when(j == 0)
                def _():
                    acc[...] = part

                @pl.when(j > 0)
                def _():
                    acc[...] += part
                return carry
            lax.fori_loop(0, T, body, 0)
            glu = acc[:, :half] * jax.nn.sigmoid(acc[:, half:])
            pad[layer, PAD:PAD + rows, h * half:(h + 1) * half] = glu.astype(bf16)

    for c in locals_:
        c.wait()
    spreads = [spread(xg, layer, x_send, x_recv) for layer in range(L)]
    spreads[0][0]()
    for c in sum(per_layer, []):
        c.wait()

    @pl.when(s < n - 1)
    def _():
        own_right(batches[0])

    @pl.when(s > 0)
    def _():
        own_left(batches[0])

    @pl.when((s == 0) & (s < n - 1))
    def _():
        for b in batches[1:]:
            own_right(b)

    @pl.when((s == n - 1) & (s > 0))
    def _():
        for b in batches[1:]:
            own_left(b)

    x_state[...] = tokens_f32(tokens, xg, t)
    drains = []

    for layer in range(L):
        first, second = 2 * layer, 2 * layer + 1
        relay(first, 0, 1)
        drains.append(spreads[layer][1]())
        normalize(layer)
        relay(first, 1, n)
        wait_across(first)
        project(layer)

        def to_right():
            return pltpu.make_async_remote_copy(
                src_ref=pad.at[layer, pl.ds(rows, PAD), :], dst_ref=pad.at[layer, pl.ds(0, PAD), :],
                send_sem=h_send.at[layer, 0], recv_sem=h_recv.at[layer, 0],
                device_id={"sp": s + 1}, device_id_type=MESH)

        def to_left():
            return pltpu.make_async_remote_copy(
                src_ref=pad.at[layer, pl.ds(PAD, PAD), :], dst_ref=pad.at[layer, pl.ds(PAD + rows, PAD), :],
                send_sem=h_send.at[layer, 1], recv_sem=h_recv.at[layer, 1],
                device_id={"sp": s - 1}, device_id_type=MESH)

        @pl.when(s < n - 1)
        def _():
            to_right().start()

        @pl.when(s > 0)
        def _():
            to_left().start()

        @pl.when(s == 0)
        def _():
            pad[layer, 0:PAD, :] = jnp.zeros((PAD, chans), bf16)

        @pl.when(s == n - 1)
        def _():
            pad[layer, PAD + rows:, :] = jnp.zeros((PAD, chans), bf16)

        relay(second, 0, 1)

        @pl.when(s > 0)
        def _():
            to_right().wait_recv()

        @pl.when(s < n - 1)
        def _():
            to_left().wait_recv()

        padf[...] = pad[layer].astype(f32)
        block = 64
        sums, squares = [], []
        for r in range(0, rows, block):
            total = jnp.zeros((block, chans), f32)
            for k in range(n_taps):
                start = r + PAD - reach + k
                total = total + taps[layer, k][None, :] * padf[start:start + block, :]
            conv[r:r + block, :] = total
            sums.append(jnp.sum(total, axis=1, keepdims=True))
            squares.append(jnp.sum(total * total, axis=1, keepdims=True))
        totals = exchange(layer, [jnp.concatenate(sums, 0), jnp.concatenate(squares, 0)])
        relay(second, 1, 2)
        total, square = totals()
        center = total / C
        spread_ = square / C - center * center
        normal = (conv[...] - center) * lax.rsqrt(spread_ + 1e-05)
        actg[layer, t] = jax.nn.silu(normal * cgain[layer][None, :]).astype(bf16)
        act_begin, act_finish = spread(actg, layer, a_send, a_recv)
        act_begin()
        drains.append(act_finish())
        relay(second, 2, n)
        wait_across(second)
        for h in range(G):
            part = None
            for j in range(T):
                term = jnp.dot(actg[layer, j], wo[layer, h, j * chans:(j + 1) * chans, :], preferred_element_type=f32)
                part = term if part is None else part + term
            cols = slice(h * out_half, (h + 1) * out_half)
            x_state[:, cols] = (x_state[:, cols] + part).astype(bf16).astype(f32)
        if layer + 1 < L:
            xg[layer + 1, t] = x_state[...].astype(bf16)
            spreads[layer + 1][0]()

        @pl.when(s < n - 1)
        def _():
            to_right().wait_send()

        @pl.when(s > 0)
        def _():
            to_left().wait_send()

    xf = x_state[...]
    totals = exchange(L, [jnp.sum(xf * xf, axis=1, keepdims=True)])

    for drain in drains:
        drain()

    def drain_step(j, carry):
        for p in range(L * pieces):
            @pl.when((j <= s) & (s < n - 1))
            def _():
                right(p, j).wait_send()

            @pl.when((j >= s) & (s > 0))
            def _():
                left(p, j).wait_send()

            @pl.when(j != s)
            def _():
                for d in range(1, G):
                    across(p, j, d, g).wait_send()
        return carry
    lax.fori_loop(0, n, drain_step, 0)

    (total,) = totals()
    scale = lax.rsqrt(total / D + 1e-06)
    result[...] = (x_state[...] * scale * fgain[...]).astype(bf16)


def tokens_f32(tokens, xg, t):
    return xg[0, t].astype(jnp.float32)


def on_device(G, n, T, tokens, norm_gain, value_w, gate_w, taps, cgain, out_w, fgain):
    L = norm_gain.shape[0]
    rows, width = tokens.shape
    depth, chans = value_w.shape[1:]
    D, C = width * T, chans * T
    bf16, f32 = jnp.bfloat16, jnp.float32
    dma = pltpu.SemaphoreType.DMA
    vmem = pl.BlockSpec(memory_space=pltpu.VMEM)
    hbm = pl.BlockSpec(memory_space=pl.ANY)
    P_ = L * (Q + 1)
    peers = max(G - 1, 1)
    return pl.pallas_call(
        functools.partial(kernel, G, n, T, L),
        out_shape=jax.ShapeDtypeStruct((rows, width), bf16),
        in_specs=[hbm, vmem, hbm, hbm, vmem, vmem, hbm, vmem],
        out_specs=vmem,
        scratch_shapes=[
            pltpu.VMEM((L, G, D, 2 * chans // G), bf16),
            pltpu.VMEM((L, G, C, width // G), bf16),
            pltpu.VMEM((L, T, rows, width), bf16),
            pltpu.VMEM((T, rows, width), bf16),
            pltpu.VMEM((rows, 2 * chans // G), f32),
            pltpu.VMEM((L, rows + 2 * PAD, chans), bf16),
            pltpu.VMEM((rows + 2 * PAD, chans), f32),
            pltpu.VMEM((rows, chans), f32),
            pltpu.VMEM((L + 1, T, 8, rows), f32),
            pltpu.VMEM((L, T, rows, chans), bf16),
            pltpu.VMEM((rows, width), f32),
            dma((1 + L * G * 3,)),
            dma((P_, n)), dma((P_, n)), dma((P_, n)),
            dma((P_, n, peers)), dma((P_, n, peers)),
            dma((L, T)), dma((L, T)), dma((L, T)), dma((L, T)),
            dma((L + 1, T)), dma((L + 1, T)),
            dma((L, 2)), dma((L, 2)),
        ],
        compiler_params=pltpu.CompilerParams(
            collective_id=0, has_side_effects=True, vmem_limit_bytes=56 * 2**20
        ),
    )(tokens, norm_gain.reshape(L * T, width), value_w, gate_w, taps, cgain, out_w, fgain.reshape(1, width))


def solution(mesh):
    placed = (
        P(("grp", "sp"), "tp"),
        P(),
        P(None, "sp", "tp"),
        P(None, "sp", "tp"),
        P(None, None, "tp"),
        P(None, "tp"),
        P(None, "sp", "tp"),
        P("tp"),
    )
    G, n, T = (mesh.shape[a] for a in ("grp", "sp", "tp"))
    return jax.shard_map(
        functools.partial(on_device, G, n, T),
        mesh=mesh, in_specs=placed, out_specs=P(("grp", "sp"), "tp"), check_vma=False,
    )
```

```python
import functools

import jax
import jax.numpy as jnp
from jax import lax
from jax.experimental import pallas as pl
from jax.experimental.pallas import tpu as pltpu
from jax.sharding import PartitionSpec as P

MESH = pl.DeviceIdType.MESH
Q = 2
PAD = 16


def kernel(
    G, n, T, L,
    tokens, gain, value_w, gate_w, taps, cgain, out_w, fgain,
    result,
    wvg, wo, xg, xn, glu_out, acc, pad, padf, conv, stat, actg, x_state,
    local_sem, z_recv, right_send, left_send, y_send, y_recv,
    x_send, x_recv, a_send, a_recv, s_send, s_recv, h_send, h_recv, f_send, f_recv,
):
    g, s, t = lax.axis_index("grp"), lax.axis_index("sp"), lax.axis_index("tp")
    rows, width = tokens.shape
    depth, chans = value_w.shape[1:]
    out_rows = out_w.shape[1]
    half = chans // G
    out_half = width // G
    reach = taps.shape[1] // 2
    n_taps = taps.shape[1]
    D = width * T
    C = chans * T
    chunk = depth // Q
    pieces = Q + 1
    f32, bf16 = jnp.float32, jnp.bfloat16
    helped = n >= 4
    last = n - 1
    is_end = (s == 0) | (s == last)
    helper = (s == 1) | (s == last - 1)
    end = jnp.where(s == 1, 0, last)
    inward = jnp.where(s == 0, 1, last - 1)

    def ends_out(p):
        return helped and p < Q

    def to_right_ok(p):
        return s < last - 1 if ends_out(p) else s < last

    def to_left_ok(p):
        return s > 1 if ends_out(p) else s > 0

    def takes(p):
        return jnp.logical_not(is_end) if ends_out(p) else s >= 0

    def by_grp(p, j):
        ok = takes(p) & (j != s)
        if helped and p == 0:
            ok = ok & jnp.logical_not((s == 1) & (j == 0)) & jnp.logical_not((s == last - 1) & (j == last))
        return ok

    def piece(p, h, j):
        layer, q = p // pieces, p % pieces
        if q < Q:
            start = pl.multiple_of(j * depth + q * chunk, chunk)
            return wvg.at[layer, h, pl.ds(start, chunk), :]
        return wo.at[layer, h, pl.ds(pl.multiple_of(j * out_rows, out_rows), out_rows), :]

    locals_ = [pltpu.make_async_copy(tokens, xg.at[0, t], local_sem.at[0])]
    own_rows = pl.ds(pl.multiple_of(s * depth, depth), depth)
    own_out = pl.ds(pl.multiple_of(s * out_rows, out_rows), out_rows)
    count = 1
    per_layer = []
    for layer in range(L):
        group = []
        for h in range(G):
            for k, w in enumerate((value_w, gate_w)):
                group.append(pltpu.make_async_copy(
                    w.at[layer, :, pl.ds(h * half, half)],
                    wvg.at[layer, h, own_rows, pl.ds(k * half, half)],
                    local_sem.at[count]))
                count += 1
            group.append(pltpu.make_async_copy(
                out_w.at[layer, :, pl.ds(h * out_half, out_half)],
                wo.at[layer, h, own_out, :], local_sem.at[count]))
            count += 1
        per_layer.append(group)
    for c in locals_ + sum(per_layer, []):
        c.start()

    barrier = pltpu.get_barrier_semaphore()
    for d in range(1, T):
        pl.semaphore_signal(barrier, inc=1, device_id={"tp": lax.rem(t + d, T)}, device_id_type=MESH)
    for d in range(1, G):
        pl.semaphore_signal(barrier, inc=1, device_id={"grp": lax.rem(g + d, G)}, device_id_type=MESH)

    @pl.when(s > 0)
    def _():
        pl.semaphore_signal(barrier, inc=1, device_id={"sp": s - 1}, device_id_type=MESH)

    @pl.when(s < n - 1)
    def _():
        pl.semaphore_signal(barrier, inc=1, device_id={"sp": s + 1}, device_id_type=MESH)

    sides = jnp.where(s > 0, 1, 0) + jnp.where(s < n - 1, 1, 0)
    pl.semaphore_wait(barrier, (T - 1) + (G - 1) + sides)

    def right(p, j):
        r = piece(p, g, j)
        return pltpu.make_async_remote_copy(
            src_ref=r, dst_ref=r, send_sem=right_send.at[p, j], recv_sem=z_recv.at[p, j],
            device_id={"sp": s + 1}, device_id_type=MESH)

    def left(p, j):
        r = piece(p, g, j)
        return pltpu.make_async_remote_copy(
            src_ref=r, dst_ref=r, send_sem=left_send.at[p, j], recv_sem=z_recv.at[p, j],
            device_id={"sp": s - 1}, device_id_type=MESH)

    def across(p, j, d, h):
        r = piece(p, h, j)
        return pltpu.make_async_remote_copy(
            src_ref=r, dst_ref=r, send_sem=y_send.at[p, j, d - 1], recv_sem=y_recv.at[p, j, d - 1],
            device_id={"grp": lax.rem(g + d, G)}, device_id_type=MESH)

    batches = []
    for layer in range(L):
        base = layer * pieces
        batches += [list(range(base, base + Q)), [base + Q]]

    def own_right(ps):
        for p in ps:
            right(p, s).start()

    def own_left(ps):
        for p in ps:
            left(p, s).start()

    def end_rows(target):
        return pltpu.make_async_remote_copy(
            src_ref=xg.at[0, t], dst_ref=xg.at[L, t], send_sem=f_send.at[0], recv_sem=f_recv.at[0],
            device_id={"sp": target}, device_id_type=MESH)

    def end_piece(d, h, j, target):
        r = piece(0, h, j)
        return pltpu.make_async_remote_copy(
            src_ref=r, dst_ref=r, send_sem=f_send.at[d], recv_sem=f_recv.at[d],
            device_id={"sp": target}, device_id_type=MESH)

    def end_glu(target):
        return pltpu.make_async_remote_copy(
            src_ref=glu_out, dst_ref=pad.at[0, pl.ds(PAD, rows), :],
            send_sem=f_send.at[G], recv_sem=f_recv.at[G],
            device_id={"sp": target}, device_id_type=MESH)

    def relay(b, low, high):
        low, high = min(low, n - 1), min(high, n - 1)
        following = batches[b + 1] if b + 1 < len(batches) else []

        def step(k, carry):
            for p in batches[b]:
                from_left, from_right = s - 1 - k, s + 1 + k

                @pl.when((from_left >= 0) & takes(p))
                def _():
                    j = jnp.maximum(from_left, 0)
                    right(p, j).wait_recv()

                    @pl.when(to_right_ok(p))
                    def _():
                        right(p, j).start()

                    @pl.when(by_grp(p, j))
                    def _():
                        for d in range(1, G):
                            across(p, j, d, g).start()

                @pl.when((from_right < n) & takes(p))
                def _():
                    j = jnp.minimum(from_right, n - 1)
                    left(p, j).wait_recv()

                    @pl.when(to_left_ok(p))
                    def _():
                        left(p, j).start()

                    @pl.when(by_grp(p, j))
                    def _():
                        for d in range(1, G):
                            across(p, j, d, g).start()

            @pl.when((k == s - 1) & (s < (last - 1 if helped and b < 2 else last)))
            def _():
                own_right(following)

            @pl.when((k == n - 2 - s) & (s > (1 if helped and b < 2 else 0)))
            def _():
                own_left(following)

            return carry

        if high > low:
            lax.fori_loop(low, high, step, 0)

    def wait_across(b):
        for p in batches[b]:
            def step(j, carry):
                @pl.when(by_grp(p, j))
                def _():
                    for d in range(1, G):
                        across(p, j, d, lax.rem(g + G - d, G)).wait_recv()
                return carry
            lax.fori_loop(0, n, step, 0)

    def spread(buf, layer, send, recv):
        def copy(bit, m):
            block = buf.at[layer, t ^ m]
            return pltpu.make_async_remote_copy(
                src_ref=block, dst_ref=block, send_sem=send.at[layer, bit + m], recv_sem=recv.at[layer, bit + m],
                device_id={"tp": t ^ bit}, device_id_type=MESH)

        def arrival(bit, m):
            block = buf.at[layer, t ^ bit ^ m]
            return pltpu.make_async_remote_copy(
                src_ref=block, dst_ref=block, send_sem=send.at[layer, bit + m], recv_sem=recv.at[layer, bit + m],
                device_id={"tp": t ^ bit}, device_id_type=MESH)

        bits = []
        bit = T // 2
        while bit >= 1:
            bits.append(bit)
            bit //= 2

        def begin():
            for bit in bits:
                copy(bit, 0).start()

        def finish():
            have, sent = [0], []
            for i, bit in enumerate(bits):
                for m in have:
                    arrival(bit, m).wait_recv()
                    sent.append((bit, m))
                    for lower in bits[i + 1:]:
                        copy(lower, m ^ bit).start()
                have = have + [m ^ bit for m in have]
            return lambda: [copy(bit, m).wait_send() for bit, m in sent]

        return begin, finish

    def exchange(index, columns):
        lane = lax.broadcasted_iota(jnp.int32, (rows, 128), 1)
        tile = jnp.zeros((rows, 128), f32)
        for i, column in enumerate(columns):
            tile = jnp.where(lane == i, column, tile)
        stat[index, 0] = tile.T[:8, :]

        def copy(d):
            return pltpu.make_async_remote_copy(
                src_ref=stat.at[index, 0], dst_ref=stat.at[index, d],
                send_sem=s_send.at[index, d - 1], recv_sem=s_recv.at[index, d - 1],
                device_id={"tp": lax.rem(t + d, T)}, device_id_type=MESH)

        for d in range(1, T):
            copy(d).start()

        def total():
            for d in range(1, T):
                copy(d).wait_recv()
            sums = stat[index, 0]
            for d in range(1, T):
                sums = sums + stat[index, d]
            wide = jnp.concatenate([sums, jnp.zeros((120, rows), f32)], axis=0).T
            for d in range(1, T):
                copy(d).wait_send()
            return [wide[:, i:i + 1] for i in range(len(columns))]

        return total

    def normalize(layer, held, into):
        def squares(j, total):
            part = xg[held, j].astype(f32)
            return total + jnp.sum(part * part, axis=1, keepdims=True)
        mean = lax.fori_loop(0, T, squares, jnp.zeros((rows, 1), f32)) / D
        scale = lax.rsqrt(mean + 1e-06)

        def body(j, carry):
            xn[into, j] = (xg[held, j].astype(f32) * scale * gain[layer * T + j][None, :]).astype(bf16)
            return carry
        lax.fori_loop(0, T, body, 0)

    def project(layer, held, put):
        for h in range(G):
            def body(j, carry):
                block = wvg[layer, h, pl.ds(pl.multiple_of(j * width, width), width), :]
                part = jnp.dot(xn[held, j], block, preferred_element_type=f32)

                @pl.when(j == 0)
                def _():
                    acc[...] = part

                @pl.when(j > 0)
                def _():
                    acc[...] += part
                return carry
            lax.fori_loop(0, T, body, 0)
            glu = acc[:, :half] * jax.nn.sigmoid(acc[:, half:])
            put(h, glu.astype(bf16))

    for c in locals_:
        c.wait()
    spreads = [spread(xg, layer, x_send, x_recv) for layer in range(L)]
    spreads[0][0]()
    for c in sum(per_layer, []):
        c.wait()

    @pl.when(to_right_ok(0))
    def _():
        own_right(batches[0])

    @pl.when(to_left_ok(0))
    def _():
        own_left(batches[0])

    if helped:
        @pl.when(is_end)
        def _():
            end_rows(inward).start()
            for d in range(1, G):
                end_piece(d, lax.rem(g + d, G), s, inward).start()

        @pl.when(s == last - 1)
        def _():
            own_right(batches[1])
            if L > 1:
                own_right(batches[2])

        @pl.when(s == 1)
        def _():
            own_left(batches[1])
            if L > 1:
                own_left(batches[2])

    @pl.when((s == 0) & (s < n - 1))
    def _():
        for b in batches[1:]:
            own_right(b)

    @pl.when((s == n - 1) & (s > 0))
    def _():
        for b in batches[1:]:
            own_left(b)

    x_state[...] = tokens_f32(tokens, xg, t)
    drains = []

    for layer in range(L):
        first, second = 2 * layer, 2 * layer + 1
        relay(first, 0, 1)
        drains.append(spreads[layer][1]())
        if helped and layer == 0:
            @pl.when(jnp.logical_not(is_end))
            def _():
                normalize(layer, layer, 0)
        else:
            normalize(layer, layer, 0)
        relay(first, 1, n)
        relay(second, 0, 1)

        def put(h, value):
            pad[layer, PAD:PAD + rows, h * half:(h + 1) * half] = value

        def put_out(h, value):
            glu_out[:, h * half:(h + 1) * half] = value

        if helped and layer == 0:
            begin, finish = spread(xg, L, x_send, x_recv)

            @pl.when(helper)
            def _():
                end_rows(end).wait_recv()
                begin()
                drain = finish()
                normalize(0, L, 1)
                for d in range(1, G):
                    end_piece(d, lax.rem(g + d, G), end, end).wait_recv()
                drain()

            wait_across(first)

            @pl.when(helper)
            def _():
                project(0, 1, put_out)
                end_glu(end).start()

            @pl.when(jnp.logical_not(is_end))
            def _():
                project(0, 0, put)

            @pl.when(helper)
            def _():
                end_glu(end).wait_send()

            @pl.when(is_end)
            def _():
                end_rows(inward).wait_send()
                for d in range(1, G):
                    end_piece(d, lax.rem(g + d, G), s, inward).wait_send()
                end_glu(inward).wait_recv()
        else:
            wait_across(first)
            project(layer, 0, put)

        def to_right():
            return pltpu.make_async_remote_copy(
                src_ref=pad.at[layer, pl.ds(rows, PAD), :], dst_ref=pad.at[layer, pl.ds(0, PAD), :],
                send_sem=h_send.at[layer, 0], recv_sem=h_recv.at[layer, 0],
                device_id={"sp": s + 1}, device_id_type=MESH)

        def to_left():
            return pltpu.make_async_remote_copy(
                src_ref=pad.at[layer, pl.ds(PAD, PAD), :], dst_ref=pad.at[layer, pl.ds(PAD + rows, PAD), :],
                send_sem=h_send.at[layer, 1], recv_sem=h_recv.at[layer, 1],
                device_id={"sp": s - 1}, device_id_type=MESH)

        @pl.when(s < n - 1)
        def _():
            to_right().start()

        @pl.when(s > 0)
        def _():
            to_left().start()

        @pl.when(s == 0)
        def _():
            pad[layer, 0:PAD, :] = jnp.zeros((PAD, chans), bf16)

        @pl.when(s == n - 1)
        def _():
            pad[layer, PAD + rows:, :] = jnp.zeros((PAD, chans), bf16)

        relay(second, 1, 2)

        @pl.when(s > 0)
        def _():
            to_right().wait_recv()

        @pl.when(s < n - 1)
        def _():
            to_left().wait_recv()

        padf[...] = pad[layer].astype(f32)
        block = 64
        sums, squares = [], []
        for r in range(0, rows, block):
            total = jnp.zeros((block, chans), f32)
            for k in range(n_taps):
                start = r + PAD - reach + k
                total = total + taps[layer, k][None, :] * padf[start:start + block, :]
            conv[r:r + block, :] = total
            sums.append(jnp.sum(total, axis=1, keepdims=True))
            squares.append(jnp.sum(total * total, axis=1, keepdims=True))
        totals = exchange(layer, [jnp.concatenate(sums, 0), jnp.concatenate(squares, 0)])
        total, square = totals()
        center = total / C
        spread_ = square / C - center * center
        normal = (conv[...] - center) * lax.rsqrt(spread_ + 1e-05)
        actg[layer, t] = jax.nn.silu(normal * cgain[layer][None, :]).astype(bf16)
        act_begin, act_finish = spread(actg, layer, a_send, a_recv)
        act_begin()
        drains.append(act_finish())
        relay(second, 2, n)
        wait_across(second)
        for h in range(G):
            part = None
            for j in range(T):
                term = jnp.dot(actg[layer, j], wo[layer, h, j * chans:(j + 1) * chans, :], preferred_element_type=f32)
                part = term if part is None else part + term
            cols = slice(h * out_half, (h + 1) * out_half)
            x_state[:, cols] = (x_state[:, cols] + part).astype(bf16).astype(f32)
        if layer + 1 < L:
            xg[layer + 1, t] = x_state[...].astype(bf16)
            spreads[layer + 1][0]()

        @pl.when(s < n - 1)
        def _():
            to_right().wait_send()

        @pl.when(s > 0)
        def _():
            to_left().wait_send()

    xf = x_state[...]
    totals = exchange(L, [jnp.sum(xf * xf, axis=1, keepdims=True)])

    for drain in drains:
        drain()

    def drain_step(j, carry):
        for p in range(L * pieces):
            came = (j == s) | takes(p)

            @pl.when((j <= s) & to_right_ok(p) & came)
            def _():
                right(p, j).wait_send()

            @pl.when((j >= s) & to_left_ok(p) & came)
            def _():
                left(p, j).wait_send()

            @pl.when(by_grp(p, j))
            def _():
                for d in range(1, G):
                    across(p, j, d, g).wait_send()
        return carry
    lax.fori_loop(0, n, drain_step, 0)

    (total,) = totals()
    scale = lax.rsqrt(total / D + 1e-06)
    result[...] = (x_state[...] * scale * fgain[...]).astype(bf16)


def tokens_f32(tokens, xg, t):
    return xg[0, t].astype(jnp.float32)


def on_device(G, n, T, tokens, norm_gain, value_w, gate_w, taps, cgain, out_w, fgain):
    L = norm_gain.shape[0]
    rows, width = tokens.shape
    depth, chans = value_w.shape[1:]
    D, C = width * T, chans * T
    bf16, f32 = jnp.bfloat16, jnp.float32
    dma = pltpu.SemaphoreType.DMA
    vmem = pl.BlockSpec(memory_space=pltpu.VMEM)
    hbm = pl.BlockSpec(memory_space=pl.ANY)
    P_ = L * (Q + 1)
    peers = max(G - 1, 1)
    return pl.pallas_call(
        functools.partial(kernel, G, n, T, L),
        out_shape=jax.ShapeDtypeStruct((rows, width), bf16),
        in_specs=[hbm, vmem, hbm, hbm, vmem, vmem, hbm, vmem],
        out_specs=vmem,
        scratch_shapes=[
            pltpu.VMEM((L, G, D, 2 * chans // G), bf16),
            pltpu.VMEM((L, G, C, width // G), bf16),
            pltpu.VMEM((L + 1, T, rows, width), bf16),
            pltpu.VMEM((2, T, rows, width), bf16),
            pltpu.VMEM((rows, chans), bf16),
            pltpu.VMEM((rows, 2 * chans // G), f32),
            pltpu.VMEM((L, rows + 2 * PAD, chans), bf16),
            pltpu.VMEM((rows + 2 * PAD, chans), f32),
            pltpu.VMEM((rows, chans), f32),
            pltpu.VMEM((L + 1, T, 8, rows), f32),
            pltpu.VMEM((L, T, rows, chans), bf16),
            pltpu.VMEM((rows, width), f32),
            dma((1 + L * G * 3,)),
            dma((P_, n)), dma((P_, n)), dma((P_, n)),
            dma((P_, n, peers)), dma((P_, n, peers)),
            dma((L + 1, T)), dma((L + 1, T)), dma((L, T)), dma((L, T)),
            dma((L + 1, T)), dma((L + 1, T)),
            dma((L, 2)), dma((L, 2)),
            dma((G + 1,)), dma((G + 1,)),
        ],
        compiler_params=pltpu.CompilerParams(
            collective_id=0, has_side_effects=True, vmem_limit_bytes=56 * 2**20
        ),
    )(tokens, norm_gain.reshape(L * T, width), value_w, gate_w, taps, cgain, out_w, fgain.reshape(1, width))


def solution(mesh):
    placed = (
        P(("grp", "sp"), "tp"),
        P(),
        P(None, "sp", "tp"),
        P(None, "sp", "tp"),
        P(None, None, "tp"),
        P(None, "tp"),
        P(None, "sp", "tp"),
        P("tp"),
    )
    G, n, T = (mesh.shape[a] for a in ("grp", "sp", "tp"))
    return jax.shard_map(
        functools.partial(on_device, G, n, T),
        mesh=mesh, in_specs=placed, out_specs=P(("grp", "sp"), "tp"), check_vma=False,
    )
```

```python
import functools

import jax
import jax.numpy as jnp
from jax import lax
from jax.experimental import pallas as pl
from jax.experimental.pallas import tpu as pltpu
from jax.sharding import PartitionSpec as P

MESH = pl.DeviceIdType.MESH
Q = 2
PAD = 16


def kernel(
    G, n, T, L,
    tokens, gain, value_w, gate_w, taps, cgain, out_w, fgain,
    result,
    wvg, wo, xg, xn, glu_out, acc, pad, padf, conv, stat, actg, x_state,
    local_sem, z_recv, right_send, left_send, y_send, y_recv,
    x_send, x_recv, a_send, a_recv, s_send, s_recv, h_send, h_recv, f_send, f_recv,
):
    g, s, t = lax.axis_index("grp"), lax.axis_index("sp"), lax.axis_index("tp")
    rows, width = tokens.shape
    depth, chans = value_w.shape[1:]
    out_rows = out_w.shape[1]
    half = chans // G
    out_half = width // G
    reach = taps.shape[1] // 2
    n_taps = taps.shape[1]
    D = width * T
    C = chans * T
    chunk = depth // Q
    pieces = Q + 1
    f32, bf16 = jnp.float32, jnp.bfloat16
    helped = n >= 4
    last = n - 1
    is_end = (s == 0) | (s == last)
    helper = (s == 1) | (s == last - 1)
    end = jnp.where(s == 1, 0, last)
    inward = jnp.where(s == 0, 1, last - 1)

    def ends_out(p):
        return helped and p < Q

    def to_right_ok(p):
        return s < last - 1 if ends_out(p) else s < last

    def to_left_ok(p):
        return s > 1 if ends_out(p) else s > 0

    def takes(p):
        return jnp.logical_not(is_end) if ends_out(p) else s >= 0

    def by_grp(p, j):
        ok = takes(p) & (j != s)
        if helped and p == 0:
            ok = ok & jnp.logical_not((s == 1) & (j == 0)) & jnp.logical_not((s == last - 1) & (j == last))
        return ok

    def piece(p, h, j):
        layer, q = p // pieces, p % pieces
        if q < Q:
            start = pl.multiple_of(j * depth + q * chunk, chunk)
            return wvg.at[layer, h, pl.ds(start, chunk), :]
        return wo.at[layer, h, pl.ds(pl.multiple_of(j * out_rows, out_rows), out_rows), :]

    locals_ = [pltpu.make_async_copy(tokens, xg.at[0, t], local_sem.at[0])]
    own_rows = pl.ds(pl.multiple_of(s * depth, depth), depth)
    own_out = pl.ds(pl.multiple_of(s * out_rows, out_rows), out_rows)
    count = 1
    per_layer = []
    for layer in range(L):
        group = []
        for h in range(G):
            for k, w in enumerate((value_w, gate_w)):
                group.append(pltpu.make_async_copy(
                    w.at[layer, :, pl.ds(h * half, half)],
                    wvg.at[layer, h, own_rows, pl.ds(k * half, half)],
                    local_sem.at[count]))
                count += 1
            group.append(pltpu.make_async_copy(
                out_w.at[layer, :, pl.ds(h * out_half, out_half)],
                wo.at[layer, h, own_out, :], local_sem.at[count]))
            count += 1
        per_layer.append(group)
    for c in locals_ + sum(per_layer, []):
        c.start()

    barrier = pltpu.get_barrier_semaphore()
    for d in range(1, T):
        pl.semaphore_signal(barrier, inc=1, device_id={"tp": lax.rem(t + d, T)}, device_id_type=MESH)
    for d in range(1, G):
        pl.semaphore_signal(barrier, inc=1, device_id={"grp": lax.rem(g + d, G)}, device_id_type=MESH)

    @pl.when(s > 0)
    def _():
        pl.semaphore_signal(barrier, inc=1, device_id={"sp": s - 1}, device_id_type=MESH)

    @pl.when(s < n - 1)
    def _():
        pl.semaphore_signal(barrier, inc=1, device_id={"sp": s + 1}, device_id_type=MESH)

    sides = jnp.where(s > 0, 1, 0) + jnp.where(s < n - 1, 1, 0)
    pl.semaphore_wait(barrier, (T - 1) + (G - 1) + sides)

    def right(p, j):
        r = piece(p, g, j)
        return pltpu.make_async_remote_copy(
            src_ref=r, dst_ref=r, send_sem=right_send.at[p, j], recv_sem=z_recv.at[p, j],
            device_id={"sp": s + 1}, device_id_type=MESH)

    def left(p, j):
        r = piece(p, g, j)
        return pltpu.make_async_remote_copy(
            src_ref=r, dst_ref=r, send_sem=left_send.at[p, j], recv_sem=z_recv.at[p, j],
            device_id={"sp": s - 1}, device_id_type=MESH)

    def across(p, j, d, h):
        r = piece(p, h, j)
        return pltpu.make_async_remote_copy(
            src_ref=r, dst_ref=r, send_sem=y_send.at[p, j, d - 1], recv_sem=y_recv.at[p, j, d - 1],
            device_id={"grp": lax.rem(g + d, G)}, device_id_type=MESH)

    batches = []
    for layer in range(L):
        base = layer * pieces
        batches += [list(range(base, base + Q)), [base + Q]]

    def own_right(ps):
        for p in ps:
            right(p, s).start()

    def own_left(ps):
        for p in ps:
            left(p, s).start()

    def end_rows(target):
        return pltpu.make_async_remote_copy(
            src_ref=xg.at[0, t], dst_ref=xg.at[L, t], send_sem=f_send.at[0], recv_sem=f_recv.at[0],
            device_id={"sp": target}, device_id_type=MESH)

    def end_piece(d, h, j, target):
        r = piece(0, h, j)
        return pltpu.make_async_remote_copy(
            src_ref=r, dst_ref=r, send_sem=f_send.at[d], recv_sem=f_recv.at[d],
            device_id={"sp": target}, device_id_type=MESH)

    def end_glu(target):
        return pltpu.make_async_remote_copy(
            src_ref=glu_out, dst_ref=pad.at[0, pl.ds(PAD, rows), :],
            send_sem=f_send.at[G], recv_sem=f_recv.at[G],
            device_id={"sp": target}, device_id_type=MESH)

    def relay(b, low, high):
        low, high = min(low, n - 1), min(high, n - 1)
        following = batches[b + 1] if b + 1 < len(batches) else []

        def step(k, carry):
            for p in batches[b]:
                from_left, from_right = s - 1 - k, s + 1 + k

                @pl.when((from_left >= 0) & takes(p))
                def _():
                    j = jnp.maximum(from_left, 0)
                    right(p, j).wait_recv()

                    @pl.when(to_right_ok(p))
                    def _():
                        right(p, j).start()

                    @pl.when(by_grp(p, j))
                    def _():
                        for d in range(1, G):
                            across(p, j, d, g).start()

                @pl.when((from_right < n) & takes(p))
                def _():
                    j = jnp.minimum(from_right, n - 1)
                    left(p, j).wait_recv()

                    @pl.when(to_left_ok(p))
                    def _():
                        left(p, j).start()

                    @pl.when(by_grp(p, j))
                    def _():
                        for d in range(1, G):
                            across(p, j, d, g).start()

            @pl.when((k == s - 1) & (s < (last - 1 if helped and b < 2 else last)))
            def _():
                own_right(following)

            @pl.when((k == n - 2 - s) & (s > (1 if helped and b < 2 else 0)))
            def _():
                own_left(following)

            return carry

        if high > low:
            lax.fori_loop(low, high, step, 0)

    def wait_across(b):
        for p in batches[b]:
            def step(j, carry):
                @pl.when(by_grp(p, j))
                def _():
                    for d in range(1, G):
                        across(p, j, d, lax.rem(g + G - d, G)).wait_recv()
                return carry
            lax.fori_loop(0, n, step, 0)

    def spread(buf, layer, send, recv):
        def copy(bit, m):
            block = buf.at[layer, t ^ m]
            return pltpu.make_async_remote_copy(
                src_ref=block, dst_ref=block, send_sem=send.at[layer, bit + m], recv_sem=recv.at[layer, bit + m],
                device_id={"tp": t ^ bit}, device_id_type=MESH)

        def arrival(bit, m):
            block = buf.at[layer, t ^ bit ^ m]
            return pltpu.make_async_remote_copy(
                src_ref=block, dst_ref=block, send_sem=send.at[layer, bit + m], recv_sem=recv.at[layer, bit + m],
                device_id={"tp": t ^ bit}, device_id_type=MESH)

        bits = []
        bit = T // 2
        while bit >= 1:
            bits.append(bit)
            bit //= 2

        def begin():
            for bit in bits:
                copy(bit, 0).start()

        def finish():
            have, sent = [0], []
            for i, bit in enumerate(bits):
                for m in have:
                    arrival(bit, m).wait_recv()
                    sent.append((bit, m))
                    for lower in bits[i + 1:]:
                        copy(lower, m ^ bit).start()
                have = have + [m ^ bit for m in have]
            return lambda: [copy(bit, m).wait_send() for bit, m in sent]

        return begin, finish

    def exchange(index, columns):
        lane = lax.broadcasted_iota(jnp.int32, (rows, 128), 1)
        tile = jnp.zeros((rows, 128), f32)
        for i, column in enumerate(columns):
            tile = jnp.where(lane == i, column, tile)
        stat[index, 0] = tile.T[:8, :]

        def copy(d):
            return pltpu.make_async_remote_copy(
                src_ref=stat.at[index, 0], dst_ref=stat.at[index, d],
                send_sem=s_send.at[index, d - 1], recv_sem=s_recv.at[index, d - 1],
                device_id={"tp": lax.rem(t + d, T)}, device_id_type=MESH)

        for d in range(1, T):
            copy(d).start()

        def total():
            for d in range(1, T):
                copy(d).wait_recv()
            sums = stat[index, 0]
            for d in range(1, T):
                sums = sums + stat[index, d]
            wide = jnp.concatenate([sums, jnp.zeros((120, rows), f32)], axis=0).T
            for d in range(1, T):
                copy(d).wait_send()
            return [wide[:, i:i + 1] for i in range(len(columns))]

        return total

    def normalize(layer, held, into):
        def squares(j, total):
            part = xg[held, j].astype(f32)
            return total + jnp.sum(part * part, axis=1, keepdims=True)
        mean = lax.fori_loop(0, T, squares, jnp.zeros((rows, 1), f32)) / D
        scale = lax.rsqrt(mean + 1e-06)

        def body(j, carry):
            xn[into, j] = (xg[held, j].astype(f32) * scale * gain[layer * T + j][None, :]).astype(bf16)
            return carry
        lax.fori_loop(0, T, body, 0)

    def project(layer, held, put):
        for h in range(G):
            def body(j, carry):
                block = wvg[layer, h, pl.ds(pl.multiple_of(j * width, width), width), :]
                part = jnp.dot(xn[held, j], block, preferred_element_type=f32)

                @pl.when(j == 0)
                def _():
                    acc[...] = part

                @pl.when(j > 0)
                def _():
                    acc[...] += part
                return carry
            lax.fori_loop(0, T, body, 0)
            glu = acc[:, :half] * jax.nn.sigmoid(acc[:, half:])
            put(h, glu.astype(bf16))

    for c in locals_:
        c.wait()
    spreads = [spread(xg, layer, x_send, x_recv) for layer in range(L)]
    spreads[0][0]()
    for c in sum(per_layer, []):
        c.wait()

    @pl.when(to_right_ok(0))
    def _():
        own_right(batches[0])

    @pl.when(to_left_ok(0))
    def _():
        own_left(batches[0])

    if helped:
        @pl.when(is_end)
        def _():
            end_rows(inward).start()
            for d in range(1, G):
                end_piece(d, lax.rem(g + d, G), s, inward).start()

        @pl.when(s == last - 1)
        def _():
            own_right(batches[1])
            if L > 1:
                own_right(batches[2])

        @pl.when(s == 1)
        def _():
            own_left(batches[1])
            if L > 1:
                own_left(batches[2])

    @pl.when((s == 0) & (s < n - 1))
    def _():
        for b in batches[1:]:
            own_right(b)

    @pl.when((s == n - 1) & (s > 0))
    def _():
        for b in batches[1:]:
            own_left(b)

    x_state[...] = tokens_f32(tokens, xg, t)
    drains = []

    for layer in range(L):
        first, second = 2 * layer, 2 * layer + 1
        if layer == 0:
            relay(first, 0, 1)
        else:
            relay(first, 1, 2)
        drains.append(spreads[layer][1]())
        if helped and layer == 0:
            @pl.when(jnp.logical_not(is_end))
            def _():
                normalize(layer, layer, 0)
        else:
            normalize(layer, layer, 0)
        relay(first, 1 if layer == 0 else 2, n)
        begin, finish = spread(xg, L, x_send, x_recv)
        if helped and layer == 0:
            @pl.when(helper)
            def _():
                end_rows(end).wait_recv()
                begin()

        relay(second, 0, 1)

        def put(h, value):
            pad[layer, PAD:PAD + rows, h * half:(h + 1) * half] = value

        def put_out(h, value):
            glu_out[:, h * half:(h + 1) * half] = value

        if helped and layer == 0:
            @pl.when(helper)
            def _():
                drain = finish()
                normalize(0, L, 1)
                for d in range(1, G):
                    end_piece(d, lax.rem(g + d, G), end, end).wait_recv()
                drain()

            wait_across(first)

            @pl.when(helper)
            def _():
                project(0, 1, put_out)
                end_glu(end).start()

            @pl.when(jnp.logical_not(is_end))
            def _():
                project(0, 0, put)

            @pl.when(helper)
            def _():
                end_glu(end).wait_send()

            @pl.when(is_end)
            def _():
                end_rows(inward).wait_send()
                for d in range(1, G):
                    end_piece(d, lax.rem(g + d, G), s, inward).wait_send()
                end_glu(inward).wait_recv()
        else:
            wait_across(first)
            project(layer, 0, put)

        def to_right():
            return pltpu.make_async_remote_copy(
                src_ref=pad.at[layer, pl.ds(rows, PAD), :], dst_ref=pad.at[layer, pl.ds(0, PAD), :],
                send_sem=h_send.at[layer, 0], recv_sem=h_recv.at[layer, 0],
                device_id={"sp": s + 1}, device_id_type=MESH)

        def to_left():
            return pltpu.make_async_remote_copy(
                src_ref=pad.at[layer, pl.ds(PAD, PAD), :], dst_ref=pad.at[layer, pl.ds(PAD + rows, PAD), :],
                send_sem=h_send.at[layer, 1], recv_sem=h_recv.at[layer, 1],
                device_id={"sp": s - 1}, device_id_type=MESH)

        @pl.when(s < n - 1)
        def _():
            to_right().start()

        @pl.when(s > 0)
        def _():
            to_left().start()

        @pl.when(s == 0)
        def _():
            pad[layer, 0:PAD, :] = jnp.zeros((PAD, chans), bf16)

        @pl.when(s == n - 1)
        def _():
            pad[layer, PAD + rows:, :] = jnp.zeros((PAD, chans), bf16)

        relay(second, 1, 2)

        @pl.when(s > 0)
        def _():
            to_right().wait_recv()

        @pl.when(s < n - 1)
        def _():
            to_left().wait_recv()

        padf[...] = pad[layer].astype(f32)
        block = 64
        sums, squares = [], []
        for r in range(0, rows, block):
            total = jnp.zeros((block, chans), f32)
            for k in range(n_taps):
                start = r + PAD - reach + k
                total = total + taps[layer, k][None, :] * padf[start:start + block, :]
            conv[r:r + block, :] = total
            sums.append(jnp.sum(total, axis=1, keepdims=True))
            squares.append(jnp.sum(total * total, axis=1, keepdims=True))
        totals = exchange(layer, [jnp.concatenate(sums, 0), jnp.concatenate(squares, 0)])
        relay(second, 2, n)
        if layer + 1 < L:
            relay(second + 1, 0, 1)
        total, square = totals()
        center = total / C
        spread_ = square / C - center * center
        normal = (conv[...] - center) * lax.rsqrt(spread_ + 1e-05)
        actg[layer, t] = jax.nn.silu(normal * cgain[layer][None, :]).astype(bf16)
        act_begin, act_finish = spread(actg, layer, a_send, a_recv)
        act_begin()
        drains.append(act_finish())
        wait_across(second)
        for h in range(G):
            part = None
            for j in range(T):
                term = jnp.dot(actg[layer, j], wo[layer, h, j * chans:(j + 1) * chans, :], preferred_element_type=f32)
                part = term if part is None else part + term
            cols = slice(h * out_half, (h + 1) * out_half)
            x_state[:, cols] = (x_state[:, cols] + part).astype(bf16).astype(f32)
        if layer + 1 < L:
            xg[layer + 1, t] = x_state[...].astype(bf16)
            spreads[layer + 1][0]()

        @pl.when(s < n - 1)
        def _():
            to_right().wait_send()

        @pl.when(s > 0)
        def _():
            to_left().wait_send()

    xf = x_state[...]
    totals = exchange(L, [jnp.sum(xf * xf, axis=1, keepdims=True)])

    for drain in drains:
        drain()

    def drain_step(j, carry):
        for p in range(L * pieces):
            came = (j == s) | takes(p)

            @pl.when((j <= s) & to_right_ok(p) & came)
            def _():
                right(p, j).wait_send()

            @pl.when((j >= s) & to_left_ok(p) & came)
            def _():
                left(p, j).wait_send()

            @pl.when(by_grp(p, j))
            def _():
                for d in range(1, G):
                    across(p, j, d, g).wait_send()
        return carry
    lax.fori_loop(0, n, drain_step, 0)

    (total,) = totals()
    scale = lax.rsqrt(total / D + 1e-06)
    result[...] = (x_state[...] * scale * fgain[...]).astype(bf16)


def tokens_f32(tokens, xg, t):
    return xg[0, t].astype(jnp.float32)


def on_device(G, n, T, tokens, norm_gain, value_w, gate_w, taps, cgain, out_w, fgain):
    L = norm_gain.shape[0]
    rows, width = tokens.shape
    depth, chans = value_w.shape[1:]
    D, C = width * T, chans * T
    bf16, f32 = jnp.bfloat16, jnp.float32
    dma = pltpu.SemaphoreType.DMA
    vmem = pl.BlockSpec(memory_space=pltpu.VMEM)
    hbm = pl.BlockSpec(memory_space=pl.ANY)
    P_ = L * (Q + 1)
    peers = max(G - 1, 1)
    return pl.pallas_call(
        functools.partial(kernel, G, n, T, L),
        out_shape=jax.ShapeDtypeStruct((rows, width), bf16),
        in_specs=[hbm, vmem, hbm, hbm, vmem, vmem, hbm, vmem],
        out_specs=vmem,
        scratch_shapes=[
            pltpu.VMEM((L, G, D, 2 * chans // G), bf16),
            pltpu.VMEM((L, G, C, width // G), bf16),
            pltpu.VMEM((L + 1, T, rows, width), bf16),
            pltpu.VMEM((2, T, rows, width), bf16),
            pltpu.VMEM((rows, chans), bf16),
            pltpu.VMEM((rows, 2 * chans // G), f32),
            pltpu.VMEM((L, rows + 2 * PAD, chans), bf16),
            pltpu.VMEM((rows + 2 * PAD, chans), f32),
            pltpu.VMEM((rows, chans), f32),
            pltpu.VMEM((L + 1, T, 8, rows), f32),
            pltpu.VMEM((L, T, rows, chans), bf16),
            pltpu.VMEM((rows, width), f32),
            dma((1 + L * G * 3,)),
            dma((P_, n)), dma((P_, n)), dma((P_, n)),
            dma((P_, n, peers)), dma((P_, n, peers)),
            dma((L + 1, T)), dma((L + 1, T)), dma((L, T)), dma((L, T)),
            dma((L + 1, T)), dma((L + 1, T)),
            dma((L, 2)), dma((L, 2)),
            dma((G + 1,)), dma((G + 1,)),
        ],
        compiler_params=pltpu.CompilerParams(
            collective_id=0, has_side_effects=True, vmem_limit_bytes=56 * 2**20
        ),
    )(tokens, norm_gain.reshape(L * T, width), value_w, gate_w, taps, cgain, out_w, fgain.reshape(1, width))


def solution(mesh):
    placed = (
        P(("grp", "sp"), "tp"),
        P(),
        P(None, "sp", "tp"),
        P(None, "sp", "tp"),
        P(None, None, "tp"),
        P(None, "tp"),
        P(None, "sp", "tp"),
        P("tp"),
    )
    G, n, T = (mesh.shape[a] for a in ("grp", "sp", "tp"))
    return jax.shard_map(
        functools.partial(on_device, G, n, T),
        mesh=mesh, in_specs=placed, out_specs=P(("grp", "sp"), "tp"), check_vma=False,
    )
```
